32 devices in a mesh: ep: 8 (over z, y), tp: 4 (over x, core).
Axes of the slice: x: 2, y: 2, z: 4, core: 2. Of those that a mesh axis runs over, the one named last changes fastest.
Arguments:
- query_rows: bfloat16 [3072, 1024], P('ep', 'tp'), may hold values from -6 to 6
- key_rows: bfloat16 [3072, 512], P('ep', 'tp'), may hold values from -6 to 6
- value_rows: bfloat16 [3072, 512], P('ep', 'tp'), may hold values from -6 to 6
- break_bias: bfloat16 [3072, 16], P('ep', 'tp'), may hold values from -14 to 0
- mixer_weight: bfloat16 [1024, 2048], P('tp'), may hold values from -0.1875 to 0.1875
- mixer_gain: bfloat16 [2048], replicated, may hold values from 0.099609375 to 1.8984375
- expert_input: bfloat16 [4096, 2048], P(('ep', 'tp')), may hold values from -6 to 6
- expert_gain: bfloat16 [2048], replicated, may hold values from 0.099609375 to 1.8984375
- route_ids: int32 [4096, 2], P('ep'), may hold values from 0 to 15, all different within a row; in each aligned block of 128 rows (0 to 127, 128 to 255, ...) at most 32 rows name the same one
- route_weights: float32 [4096, 2], P(('ep', 'tp')), may hold values from 0.2 to 2
- expert_gate: bfloat16 [16, 2048, 2048], P('ep', None, 'tp'), may hold values from -0.125 to 0.125
- expert_up: bfloat16 [16, 2048, 2048], P('ep', None, 'tp'), may hold values from -0.125 to 0.125
- expert_down: bfloat16 [16, 2048, 2048], P('ep', 'tp'), may hold values from -0.125 to 0.125
- shared_gate: bfloat16 [2048, 512], replicated, may hold values from -0.125 to 0.125
- shared_up: bfloat16 [2048, 512], replicated, may hold values from -0.125 to 0.125
- shared_down: bfloat16 [512, 2048], replicated, may hold values from -0.25 to 0.25
Outputs:
- mixer_out: bfloat16 [3072, 2048], P(('ep', 'tp'))
- expert_out: bfloat16 [4096, 2048], P(('ep', 'tp'))
The draws below stay inside these ranges and needn't reach their ends.
Inputs may be any that keep to these rules, and one draw needn't show every extreme that they name: `route_ids`: each row names 2 different experts. Within the rows of one device no expert is named more than 32 times, and in every draw some expert is named exactly 32 times within the rows of some device.
All inputs are finite; a program needn't handle non-finite values.
Results may differ from the reference program's by a relative error of at most 0.012.
Values may be sent and summed in bfloat16 or wider, within the bound.
A program may use at most 192 MiB of HBM per device.

```python
import math
import jax
import jax.numpy as jnp
import numpy as np
from jax import lax

D = 2048
DH = 64
HEADS = 16
KV_HEADS = 8
FF_E = 2048
SHARED_FF = 512
TOPK = 2
SEQS = 1
TOK_A_DEV = 384
TOK_B_DEV = 128
EXPERTS = 16
CAP = 32
ATTENTION_TOKENS = 3072
SEQUENCE_LENGTH = 3072
TOKENS_B = 4096
N_EP = 8
N_TP = 4


def draw_break_bias(key, part):
    head_random_key, perturb_random_key, block_random_key, spike_random_key, noise_random_key = jax.random.split(jax.random.fold_in(key, 17), 5)
    slow_share = 0.5
    slow = jax.random.uniform(head_random_key, (HEADS,)) < slow_share
    base = jnp.where(slow, jnp.log(0.8 / SEQUENCE_LENGTH), jnp.log(1.0 / 40.0))
    base = base + 0.3 * jax.random.normal(perturb_random_key, (HEADS,))
    blocks = jax.random.uniform(block_random_key, (ATTENTION_TOKENS // TOK_A_DEV, 1), minval=-1.05, maxval=1.05)
    magnitude_level = jnp.repeat(blocks, TOK_A_DEV, axis=0) + base[None, :]
    spike_batch = jax.random.uniform(spike_random_key, (ATTENTION_TOKENS, 1)) < 4.0 / SEQUENCE_LENGTH
    magnitude_level = jnp.where(spike_batch, -0.8, magnitude_level)
    magnitude_level = magnitude_level + 0.3 * jax.random.normal(noise_random_key, (ATTENTION_TOKENS, HEADS))
    return jnp.clip(magnitude_level, -14.0, 0.0).astype(jnp.bfloat16)


def block_scale(key, dims, cuts, least, high):
    def one(position, shards_of):
        heights = jax.random.uniform(jax.random.fold_in(jax.random.fold_in(key, 6), position), (shards_of,), jnp.float32, least / len(cuts), high / len(cuts))
        return jnp.repeat(jnp.exp(heights), dims[position] // shards_of).reshape((-1,) + (1,) * (len(dims) - position - 1))

    factor_of = one(*cuts[0])
    for cut in cuts[1:]:
        factor_of = factor_of * one(*cut)
    return factor_of


def deal_out(own_key, own, number, rows, number_of, top, most, skew):
    ranking = jax.random.permutation(own_key, number_of)
    packed, common = portions_of(number_of, rows * top, most, skew, True), portions_of(number_of, rows * top, most, skew, False)
    places = jnp.arange(number_of)

    def named(sizes, turn):
        used = int((sizes > 0).sum())
        fixed = max(1, used // 4)
        passed = fixed + (places - fixed + turn * (used - fixed)) % max(1, number_of - fixed)
        return jnp.zeros((number_of,), jnp.int32).at[ranking[jnp.where(places < fixed, places, passed)]].set(jnp.asarray(sizes, jnp.int32))

    sizes = jnp.where(number % 4 == 0, named(packed, number // 4), named(common, number - number // 4 - 1))
    mixed = jax.random.permutation(jax.random.fold_in(own, 3), number_of)
    giver, sink = mixed[0:number_of // 2 * 2:2], mixed[1:number_of // 2 * 2:2]
    slack = jnp.minimum(sizes[giver] - 1, most - sizes[sink]) // 2
    slack = jnp.where((giver == ranking[0]) | (sink == ranking[0]) | (sizes[sink] == 0), 0, jnp.maximum(slack, 0))
    passed = jax.random.randint(jax.random.fold_in(own, 4), (number_of // 2,), 0, 1 << 20) % (slack + 1)
    sizes = sizes.at[giver].add(-passed).at[sink].add(passed)
    labels = jnp.searchsorted(jnp.cumsum(sizes), jnp.arange(rows * top), side="right").astype(jnp.int32)
    listing = labels.reshape(top, rows).T
    listing = listing[jax.random.permutation(jax.random.fold_in(own, 1), rows)]
    turn = jax.random.randint(jax.random.fold_in(own, 2), (rows, 1), 0, top)
    return jnp.take_along_axis(listing, (jnp.arange(top)[None, :] + turn) % top, axis=1)


def portions_of(number_of, total, most, skew, full):
    loads = [(1 << 20) // math.isqrt(rank ** skew) + 1 for rank in range(1, number_of + 1)]
    largest = most if full else min(most, max(-(-total // number_of), total * loads[0] // sum(loads)))
    least = 1 if total - largest >= number_of - 1 else 0
    holding, rest = [largest] + [least] * (number_of - 1), total - largest - least * (number_of - 1)
    while rest > 0:
        free = [i for i in range(1, number_of) if holding[i] < largest] or [i for i in range(1, number_of) if holding[i] < most]
        pool, remaining = sum([loads[i] for i in free]), rest
        for i in free:
            addition = min(most - holding[i], max(1, remaining * loads[i] // pool), rest)
            holding[i] = holding[i] + addition
            rest = rest - addition
    return np.array(holding)


def gaussian(stream_key, extent, width, limit, cuts=(), kind=jnp.bfloat16):
    level = block_scale(stream_key, extent, cuts, -0.22, 0.18) if cuts else 1.0
    values = jax.random.normal(stream_key, extent, jnp.float32) * width * level
    return jnp.minimum(jnp.maximum(values, -limit), limit).astype(kind)


def setup_inputs(seed: int = 0) -> dict:
    arg_keys = jax.random.split(jax.random.key(seed), 17)
    query_rows = gaussian(arg_keys[0], (ATTENTION_TOKENS, HEADS * DH), 1.0, 6.0, ((0, 8), (1, 4)))
    key_rows = gaussian(arg_keys[1], (ATTENTION_TOKENS, KV_HEADS * DH), 1.0, 6.0, ((0, 8), (1, 4)))
    value_rows = gaussian(arg_keys[2], (ATTENTION_TOKENS, KV_HEADS * DH), 1.0, 6.0, ((0, 8), (1, 4)))
    break_bias = draw_break_bias(jax.random.fold_in(arg_keys[16], 71), 0)
    mixer_weight = gaussian(arg_keys[4], (HEADS * DH, D), (HEADS * DH) ** -0.5, 0.1875, ((0, 4),))
    mixer_gain = jnp.clip(1.0 + 0.18 * jax.random.normal(arg_keys[5], (D,), jnp.float32), 0.099609375, 1.8984375).astype(jnp.bfloat16)
    expert_input = gaussian(arg_keys[6], (TOKENS_B, D), 1.0, 6.0, ((0, 32),))
    expert_gain = jnp.clip(1.0 + 0.18 * jax.random.normal(arg_keys[7], (D,), jnp.float32), 0.099609375, 1.8984375).astype(jnp.bfloat16)
    route_ids_keys = jax.random.split(jax.random.fold_in(arg_keys[8], 1), TOKENS_B // TOK_B_DEV)
    route_ids_turns = jax.random.permutation(jax.random.fold_in(arg_keys[8], 3), TOKENS_B // TOK_B_DEV)
    route_ids = jax.vmap(lambda own, number: deal_out(jax.random.fold_in(arg_keys[8], 2), own, number, TOK_B_DEV, EXPERTS, TOPK, CAP, 1))(route_ids_keys, route_ids_turns).reshape((TOKENS_B, TOPK))
    route_weights = jnp.clip(jnp.exp(math.log(2.0) - 2.3025851 * jax.random.uniform(arg_keys[9], (TOKENS_B, TOPK), jnp.float32) ** block_scale(arg_keys[9], (TOKENS_B, TOPK), ((0, 32),), -0.2, 0.2)), 0.2, 2.0)
    expert_gate = gaussian(arg_keys[10], (EXPERTS, D, FF_E), D ** -0.5, 0.125, ((0, 8), (2, 4)))
    expert_up = gaussian(arg_keys[11], (EXPERTS, D, FF_E), D ** -0.5, 0.125, ((0, 8), (2, 4)))
    expert_down = gaussian(arg_keys[12], (EXPERTS, FF_E, D), FF_E ** -0.5, 0.125, ((0, 8), (1, 4)))
    shared_gate = gaussian(arg_keys[13], (D, SHARED_FF), D ** -0.5, 0.125)
    shared_up = gaussian(arg_keys[14], (D, SHARED_FF), D ** -0.5, 0.125)
    shared_down = gaussian(arg_keys[15], (SHARED_FF, D), SHARED_FF ** -0.5, 0.25)
    return dict(query_rows=query_rows, key_rows=key_rows, value_rows=value_rows, break_bias=break_bias, mixer_weight=mixer_weight, mixer_gain=mixer_gain, expert_input=expert_input, expert_gain=expert_gain, route_ids=route_ids, route_weights=route_weights, expert_gate=expert_gate, expert_up=expert_up, expert_down=expert_down, shared_gate=shared_gate, shared_up=shared_up, shared_down=shared_down)


norm_eps = 1e-06

def rms_scale(values, gain):
    values = values.astype(jnp.float32)
    scale = lax.rsqrt(lax.optimization_barrier(jnp.mean(values * values, axis=-1, keepdims=True)) + norm_eps)
    return (values * scale * gain.astype(jnp.float32)).astype(jnp.bfloat16)

def rounded(values):
    return lax.optimization_barrier(values.astype(jnp.bfloat16)).astype(jnp.float32)

def mixer_reference(query_rows, key_rows, value_rows, break_bias, mixer_weight, mixer_gain):
    groups = HEADS // KV_HEADS
    span_shards = N_EP // SEQS
    queries = query_rows.astype(jnp.float32).reshape(N_EP, TOK_A_DEV, KV_HEADS, groups, DH)
    keys = key_rows.astype(jnp.float32).reshape(N_EP, TOK_A_DEV, KV_HEADS, DH)
    values = value_rows.astype(jnp.float32).reshape(N_EP, TOK_A_DEV, KV_HEADS, DH)
    biases = break_bias.astype(jnp.float32).reshape(N_EP, TOK_A_DEV, HEADS)
    offsets = jnp.arange(TOK_A_DEV, dtype=jnp.int32)

    def query_block(device):
        query_block_rows = lax.dynamic_index_in_dim(queries, device, 0, keepdims=False)
        query_pos = device * TOK_A_DEV + offsets

        def visit(carry, shard):
            output, later = carry

            def compute(unused):
                key_block = lax.dynamic_index_in_dim(keys, shard, 0, keepdims=False)
                value_block = lax.dynamic_index_in_dim(values, shard, 0, keepdims=False)
                bias_block = lax.dynamic_index_in_dim(biases, shard, 0, keepdims=False)
                scores = jnp.einsum('rkgd,skd->kgrs', query_block_rows, key_block)
                scores = scores.reshape(HEADS, TOK_A_DEV, TOK_A_DEV) * DH ** (-0.5)
                scores = scores + bias_block.T[:, None, :]
                key_pos = shard * TOK_A_DEV + offsets
                visible = key_pos[None, :] < query_pos[:, None]
                keep = jnp.where(visible, -jax.nn.softplus(scores), 0.0)
                beyond = lax.cumsum(keep, axis=2, reverse=True) - keep
                weights = jnp.where(visible, jnp.exp(jax.nn.log_sigmoid(scores) + beyond), 0.0)
                weights = rounded(weights).reshape(KV_HEADS, groups, TOK_A_DEV, TOK_A_DEV)
                block_sum = jnp.einsum('kgrs,skd->kgrd', weights, value_block).reshape(HEADS, TOK_A_DEV, DH)
                return (output + jnp.exp(later)[:, :, None] * block_sum, later + lax.optimization_barrier(jnp.sum(keep, axis=2)))
            wanted = (shard <= device) & (shard // span_shards == device // span_shards)
            return (lax.cond(wanted, compute, lambda unused: (output, later), None), None)
        initial = (jnp.zeros((HEADS, TOK_A_DEV, DH), jnp.float32), jnp.zeros((HEADS, TOK_A_DEV), jnp.float32))
        (output, later), unused = lax.scan(visit, initial, jnp.arange(N_EP - 1, -1, -1, dtype=jnp.int32))
        return output.transpose(1, 0, 2).reshape(TOK_A_DEV, HEADS * DH)
    attended = lax.map(query_block, jnp.arange(N_EP, dtype=jnp.int32))
    attended = attended.reshape(ATTENTION_TOKENS, HEADS * DH).astype(jnp.bfloat16)
    group_width = HEADS * DH // N_TP
    projected = jnp.zeros((ATTENTION_TOKENS, D), jnp.float32)
    for group in range(N_TP):
        lower = group * group_width
        upper = lower + group_width
        projected = projected + rounded(jnp.dot(attended[:, lower:upper], mixer_weight[lower:upper], preferred_element_type=jnp.float32))
    return rms_scale(projected, mixer_gain)

def expert_reference(expert_input, expert_gain, route_ids, route_weights, expert_gate, expert_up, expert_down, shared_gate, shared_up, shared_down):
    normed = rms_scale(expert_input, expert_gain)
    padded = jnp.concatenate([normed, jnp.zeros((1, D), jnp.bfloat16)], axis=0)
    quarter = FF_E // N_TP
    slot_count = N_EP * N_TP * CAP

    def one_expert(routed, expert):
        named = route_ids == expert
        owners = jnp.nonzero(jnp.any(named, axis=1), size=slot_count, fill_value=TOKENS_B)[0].astype(jnp.int32)
        arrived = padded[owners]
        gate_proj = jnp.dot(arrived, expert_gate[expert], preferred_element_type=jnp.float32)
        up_proj = jnp.dot(arrived, expert_up[expert], preferred_element_type=jnp.float32)
        hidden = (jax.nn.silu(gate_proj) * up_proj).astype(jnp.bfloat16)
        down_matrix = expert_down[expert]
        output = jnp.zeros((slot_count, D), jnp.float32)
        for group in range(N_TP):
            lower = group * quarter
            upper = lower + quarter
            output = output + rounded(jnp.dot(hidden[:, lower:upper], down_matrix[lower:upper], preferred_element_type=jnp.float32))
        output = rounded(output)
        weight = lax.optimization_barrier(jnp.sum(jnp.where(named, route_weights, 0.0), axis=1))
        weight = jnp.concatenate([weight, jnp.zeros((1,), jnp.float32)], axis=0)
        return (routed.at[owners].add(weight[owners][:, None] * output), None)
    routed, unused = lax.scan(one_expert, jnp.zeros((TOKENS_B + 1, D), jnp.float32), jnp.arange(EXPERTS, dtype=jnp.int32))
    shared_hidden = (jax.nn.silu(jnp.dot(normed, shared_gate, preferred_element_type=jnp.float32)) * jnp.dot(normed, shared_up, preferred_element_type=jnp.float32)).astype(jnp.bfloat16)
    total = routed[:TOKENS_B] + jnp.dot(shared_hidden, shared_down, preferred_element_type=jnp.float32)
    return total.astype(jnp.bfloat16)

def reference(query_rows, key_rows, value_rows, break_bias, mixer_weight, mixer_gain, expert_input, expert_gain, route_ids, route_weights, expert_gate, expert_up, expert_down, shared_gate, shared_up, shared_down):
    mixer_out = mixer_reference(query_rows, key_rows, value_rows, break_bias, mixer_weight, mixer_gain)
    expert_out = expert_reference(expert_input, expert_gain, route_ids, route_weights, expert_gate, expert_up, expert_down, shared_gate, shared_up, shared_down)
    return (mixer_out, expert_out)
```

```python
import functools

import jax
import jax.numpy as jnp
from jax import lax
from jax.experimental import pallas as pl
from jax.experimental.pallas import tpu as pltpu
from jax.sharding import PartitionSpec as P


DH = 64
TOPK = 2
SEQS = 1


norm_eps = 1e-06


def rms_scale(values, gain):
    values = values.astype(jnp.float32)
    scale = lax.rsqrt(jnp.mean(values * values, axis=-1, keepdims=True) + norm_eps)
    return (values * scale * gain.astype(jnp.float32)).astype(jnp.bfloat16)


def attention_kernel(span_shards, place_ref, query_ref, key_ref, value_ref, bias_ref, out_ref):
    rows = query_ref.shape[1]
    device = place_ref[0]
    first = (device // span_shards) * span_shards
    queries = query_ref[0]
    row_of = lax.broadcasted_iota(jnp.int32, (rows, rows), 0)
    column_of = lax.broadcasted_iota(jnp.int32, (rows, rows), 1)
    visible = column_of < row_of
    after = visible.astype(jnp.float32).astype(jnp.bfloat16)

    def visit(shard, diagonal):
        start = pl.multiple_of(shard * rows, rows)
        keys = key_ref[pl.ds(start, rows), :]
        values = value_ref[pl.ds(start, rows), :]
        scores = lax.dot_general(
            queries, keys, (((1,), (1,)), ((), ())), preferred_element_type=jnp.float32
        )
        scores = scores + bias_ref[0, pl.ds(shard, 1), :]
        soft = jnp.log(1.0 + jnp.exp(-jnp.abs(scores)))
        keep = -(jnp.maximum(scores, 0.0) + soft)
        if diagonal:
            keep = jnp.where(visible, keep, 0.0)
        high = keep.astype(jnp.bfloat16)
        low = (keep - high.astype(jnp.float32)).astype(jnp.bfloat16)
        beyond = jnp.dot(high, after, preferred_element_type=jnp.float32) + jnp.dot(
            low, after, preferred_element_type=jnp.float32
        )
        weights = jnp.exp(jnp.minimum(scores, 0.0) - soft + beyond)
        if diagonal:
            weights = jnp.where(visible, weights, 0.0)
        total = beyond[:, 0:1] + keep[:, 0:1]
        summed = jnp.dot(weights.astype(jnp.bfloat16), values, preferred_element_type=jnp.float32)
        return summed, total

    output, later = visit(device, True)

    def earlier(step, current):
        output, later = current
        summed, total = visit(device - 1 - step, False)
        return output + jnp.exp(later) * summed, later + total

    output, later = lax.fori_loop(0, device - first, earlier, (output, later))
    out_ref[0] = output.astype(jnp.bfloat16)


def attend(query_rows, gathered, kv_width, heads_local, kv_local, span_shards, ep_size):
    rows = query_rows.shape[0]
    groups = heads_local // kv_local
    tokens = gathered.shape[0]
    keys = gathered[:, :kv_width]
    values = gathered[:, kv_width : 2 * kv_width]
    biases = gathered[:, 2 * kv_width : 2 * kv_width + heads_local].astype(jnp.float32).T
    biases = biases.reshape(heads_local, tokens // rows, rows)
    queries = (query_rows * jnp.bfloat16(DH ** (-0.5))).reshape(rows, heads_local, DH)
    queries = queries.transpose(1, 0, 2)
    place = jnp.arange(kv_width, dtype=jnp.int32) // DH
    owned = place[None, :] == (jnp.arange(heads_local, dtype=jnp.int32) // groups)[:, None]
    padded = jnp.where(owned[:, None, :], jnp.tile(queries, (1, 1, kv_local)), 0)
    device = lax.axis_index("ep").astype(jnp.int32).reshape(1)
    blocks = (ep_size + 1) // 2 * heads_local
    output = pl.pallas_call(
        functools.partial(attention_kernel, span_shards),
        out_shape=jax.ShapeDtypeStruct((heads_local, rows, kv_width), jnp.bfloat16),
        grid=(heads_local,),
        in_specs=[
            pl.BlockSpec(memory_space=pltpu.SMEM),
            pl.BlockSpec((1, rows, kv_width), lambda h: (h, 0, 0)),
            pl.BlockSpec((tokens, kv_width), lambda h: (0, 0)),
            pl.BlockSpec((tokens, kv_width), lambda h: (0, 0)),
            pl.BlockSpec((1, tokens // rows, rows), lambda h: (h, 0, 0)),
        ],
        out_specs=pl.BlockSpec((1, rows, kv_width), lambda h: (h, 0, 0)),
        compiler_params=pltpu.CompilerParams(
            dimension_semantics=("arbitrary",), vmem_limit_bytes=32 * 1024 * 1024
        ),
        cost_estimate=pl.CostEstimate(
            flops=40 * 2 * blocks * rows * rows * rows,
            bytes_accessed=4 * tokens * kv_width,
            transcendentals=3 * blocks * rows * rows,
        ),
        name="attention",
    )(device, padded, keys, values, biases)
    picked = [
        output[head, :, (head // groups) * DH : (head // groups + 1) * DH]
        for head in range(heads_local)
    ]
    return jnp.concatenate(picked, axis=1)


def on_device(
    query_rows,
    key_rows,
    value_rows,
    break_bias,
    mixer_weight,
    mixer_gain,
    expert_input,
    expert_gain,
    route_ids,
    route_weights,
    expert_gate,
    expert_up,
    expert_down,
    shared_gate,
    shared_up,
    shared_down,
):
    heads_local = query_rows.shape[1] // DH
    kv_width = key_rows.shape[1]
    kv_local = kv_width // DH
    ep_size = lax.axis_size("ep")
    span_shards = ep_size // SEQS
    bias_pad = (-heads_local) % 128
    own_terms = jnp.concatenate(
        [key_rows, value_rows, jnp.pad(break_bias, ((0, 0), (0, bias_pad)))], axis=1
    )
    gathered = lax.all_gather(own_terms, "ep", axis=0, tiled=True)

    token_count = expert_input.shape[0]
    local_experts = expert_gate.shape[0]
    experts_all = local_experts * ep_size
    capacity = 2 * token_count * TOPK // experts_all
    slots = ep_size * capacity
    tp_index = lax.axis_index("tp")
    normed = rms_scale(expert_input, expert_gain)
    ids = lax.dynamic_slice_in_dim(route_ids, tp_index * token_count, token_count, 0)
    flat = ids.reshape(-1)
    onehot = (flat[:, None] == jnp.arange(experts_all, dtype=jnp.int32)[None, :]).astype(jnp.int32)
    before = jnp.cumsum(onehot, axis=0) - onehot
    rank = jnp.sum(before * onehot, axis=1).reshape(token_count, TOPK)
    position = (ids // local_experts) * capacity + rank
    slot_range = jnp.arange(slots, dtype=jnp.int32)
    arrived, mixing = [], []
    for expert in range(local_experts):
        slot_of = jnp.where(ids % local_experts == expert, position, -1)
        named = slot_of[:, :, None] == slot_range[None, None, :]
        chosen = jnp.any(named, axis=1).astype(jnp.bfloat16)
        weight = jnp.sum(jnp.where(named, route_weights[:, :, None], 0.0), axis=1)
        high = weight.astype(jnp.bfloat16)
        low = (weight - high.astype(jnp.float32)).astype(jnp.bfloat16)
        mixing.append((high, low))
        outgoing = lax.dot_general(
            chosen, normed, (((0,), (0,)), ((), ())), preferred_element_type=jnp.float32
        ).astype(jnp.bfloat16)
        arrived.append(lax.all_to_all(outgoing, "ep", split_axis=0, concat_axis=0, tiled=True))
    pieces = [lax.all_gather(rows, "tp", axis=0, tiled=True) for rows in arrived]

    attended = attend(
        query_rows, gathered, kv_width, heads_local, kv_local, span_shards, ep_size
    )
    shared_hidden = (
        jax.nn.silu(jnp.dot(normed, shared_gate, preferred_element_type=jnp.float32))
        * jnp.dot(normed, shared_up, preferred_element_type=jnp.float32)
    ).astype(jnp.bfloat16)
    expert_out = jnp.dot(shared_hidden, shared_down, preferred_element_type=jnp.float32)
    expert_out = lax.optimization_barrier(expert_out)

    returned = []
    for expert in range(local_experts):
        piece = pieces[expert]
        gate_proj = jnp.dot(piece, expert_gate[expert], preferred_element_type=jnp.float32)
        up_proj = jnp.dot(piece, expert_up[expert], preferred_element_type=jnp.float32)
        hidden = (jax.nn.silu(gate_proj) * up_proj).astype(jnp.bfloat16)
        part = jnp.dot(hidden, expert_down[expert], preferred_element_type=jnp.float32)
        summed = lax.psum_scatter(
            part.astype(jnp.bfloat16), "tp", scatter_dimension=0, tiled=True
        )
        returned.append(lax.all_to_all(summed, "ep", split_axis=0, concat_axis=0, tiled=True))
    projected = lax.psum_scatter(
        jnp.dot(attended, mixer_weight, preferred_element_type=jnp.float32).astype(jnp.bfloat16),
        "tp",
        scatter_dimension=0,
        tiled=True,
    ).astype(jnp.float32)
    mixer_out = rms_scale(projected, mixer_gain)
    for (high, low), results in zip(mixing, returned):
        expert_out = (
            expert_out
            + jnp.dot(high, results, preferred_element_type=jnp.float32)
            + jnp.dot(low, results, preferred_element_type=jnp.float32)
        )
    return (mixer_out, expert_out.astype(jnp.bfloat16))


def solution(mesh):
    return jax.shard_map(
        on_device,
        mesh=mesh,
        in_specs=(
            P("ep", "tp"),
            P("ep", "tp"),
            P("ep", "tp"),
            P("ep", "tp"),
            P("tp", None),
            P(),
            P(("ep", "tp"), None),
            P(),
            P("ep", None),
            P(("ep", "tp"), None),
            P("ep", None, "tp"),
            P("ep", None, "tp"),
            P("ep", "tp", None),
            P(),
            P(),
            P(),
        ),
        out_specs=(P(("ep", "tp"), None), P(("ep", "tp"), None)),
        check_vma=False,
    )
```
